32 devices in a mesh: gr: 2 (over x), fs: 4 (over z), tp: 4 (over y, core).
Axes of the slice: x: 2, y: 2, z: 4, core: 2. Of those that a mesh axis runs over, the one named last changes fastest.
Arguments:
- prompt: bfloat16 [4096, 2048], P(('gr', 'fs')), may hold values from -6 to 6
- gain_first: float32 [2048], P(('gr', 'fs')), may hold values from 0.1 to 1.9
- gate_first: float32 [2048, 2816], P(('gr', 'fs'), 'tp'), may hold values from -0.125 to 0.125
- up_first: float32 [2048, 2816], P(('gr', 'fs'), 'tp'), may hold values from -0.125 to 0.125
- down_first: float32 [2816, 2048], P(('gr', 'fs'), 'tp'), may hold values from -0.109375 to 0.109375
- gain_second: float32 [2048], P(('gr', 'fs')), may hold values from 0.1 to 1.9
- gate_second: float32 [2048, 2816], P(('gr', 'fs'), 'tp'), may hold values from -0.125 to 0.125
- up_second: float32 [2048, 2816], P(('gr', 'fs'), 'tp'), may hold values from -0.125 to 0.125
- down_second: float32 [2816, 2048], P(('gr', 'fs'), 'tp'), may hold values from -0.109375 to 0.109375
Outputs:
- serve_gate_first: bfloat16 [2048, 2816], P(None, 'tp')
- serve_up_first: bfloat16 [2048, 2816], P(None, 'tp')
- serve_down_first: bfloat16 [2816, 2048], P('tp')
- serve_gate_second: bfloat16 [2048, 2816], P(None, 'tp')
- serve_up_second: bfloat16 [2048, 2816], P(None, 'tp')
- serve_down_second: bfloat16 [2816, 2048], P('tp')
- mixed: bfloat16 [4096, 2048], P(('gr', 'fs', 'tp'))
The draws below stay inside these ranges and needn't reach their ends.
All inputs are finite; a program needn't handle non-finite values.
Results may differ from the reference program's by a relative error of at most 0.0085.
Values may be sent and summed in bfloat16 or wider, within the bound.
A program may use at most 128 MiB of HBM per device.

```python
import jax
import jax.numpy as jnp
from jax import lax

D = 2048
FF = 2816
TOKENS = 4096
N_TP = 4


def shard_levels(stream_key, dims, pieces, low, high):
    def one(dim, shards_of):
        steps = jax.random.uniform(jax.random.fold_in(jax.random.fold_in(stream_key, 6), dim), (shards_of,), jnp.float32, low / len(pieces), high / len(pieces))
        return jnp.repeat(jnp.exp(steps), dims[dim] // shards_of).reshape((-1,) + (1,) * (len(dims) - dim - 1))

    level = one(*pieces[0])
    for cut in pieces[1:]:
        level = level * one(*cut)
    return level


def normal_values(stream_key, shape, scale, most, pieces=(), dtype=jnp.bfloat16):
    gain = shard_levels(stream_key, shape, pieces, -0.22, 0.18) if pieces else 1.0
    result = jax.random.normal(stream_key, shape, jnp.float32) * scale * gain
    return jnp.minimum(jnp.maximum(result, -most), most).astype(dtype)


def setup_inputs(seed: int = 0) -> dict:
    keys = jax.random.split(jax.random.key(seed), 10)
    prompt = normal_values(keys[0], (TOKENS, D), 1.0, 6.0, ((0, 8),))
    gain_first = jnp.clip(1.0 + 0.18 * jax.random.normal(keys[1], (D,), jnp.float32), 0.1, 1.9)
    gate_first = normal_values(keys[2], (D, FF), D ** -0.5, 0.125, ((0, 8), (1, 4)), jnp.float32)
    up_first = normal_values(keys[3], (D, FF), D ** -0.5, 0.125, ((0, 8), (1, 4)), jnp.float32)
    down_first = normal_values(keys[4], (FF, D), FF ** -0.5, 0.109375, ((0, 8), (1, 4)), jnp.float32)
    gain_second = jnp.clip(1.0 + 0.18 * jax.random.normal(keys[5], (D,), jnp.float32), 0.1, 1.9)
    gate_second = normal_values(keys[6], (D, FF), D ** -0.5, 0.125, ((0, 8), (1, 4)), jnp.float32)
    up_second = normal_values(keys[7], (D, FF), D ** -0.5, 0.125, ((0, 8), (1, 4)), jnp.float32)
    down_second = normal_values(keys[8], (FF, D), FF ** -0.5, 0.109375, ((0, 8), (1, 4)), jnp.float32)
    return dict(prompt=prompt, gain_first=gain_first, gate_first=gate_first, up_first=up_first, down_first=down_first, gain_second=gain_second, gate_second=gate_second, up_second=up_second, down_second=down_second)


def normalize(rows):
    rows = rows.astype(jnp.float32)
    scale = jax.lax.rsqrt(lax.optimization_barrier(jnp.mean(rows * rows, axis=-1, keepdims=True)) + 1e-06)
    return (rows * scale).astype(jnp.bfloat16)

def layer_branch(normed, w_gate, w_up, w_down):
    gate = jnp.dot(normed, w_gate, preferred_element_type=jnp.float32)
    upper = jnp.dot(normed, w_up, preferred_element_type=jnp.float32)
    hidden = (jax.nn.silu(gate) * upper).astype(jnp.bfloat16)
    width = hidden.shape[1] // N_TP
    total = jnp.zeros((hidden.shape[0], w_down.shape[1]), jnp.float32)
    for block in range(N_TP):
        part = jnp.dot(hidden[:, block * width:(block + 1) * width], w_down[block * width:(block + 1) * width, :], preferred_element_type=jnp.float32)
        total = total + part.astype(jnp.bfloat16).astype(jnp.float32)
    return total

def reference(prompt, gain_first, gate_first, up_first, down_first, gain_second, gate_second, up_second, down_second):
    serve_gate_first = (gain_first[:, None] * gate_first).astype(jnp.bfloat16)
    serve_up_first = (gain_first[:, None] * up_first).astype(jnp.bfloat16)
    serve_down_first = down_first.astype(jnp.bfloat16)
    serve_gate_second = (gain_second[:, None] * gate_second).astype(jnp.bfloat16)
    serve_up_second = (gain_second[:, None] * up_second).astype(jnp.bfloat16)
    serve_down_second = down_second.astype(jnp.bfloat16)
    stream = prompt.astype(jnp.float32) + 0.5 * layer_branch(normalize(prompt), serve_gate_first, serve_up_first, serve_down_first)
    mixed = (stream + 0.5 * layer_branch(normalize(stream), serve_gate_second, serve_up_second, serve_down_second)).astype(jnp.bfloat16)
    return (serve_gate_first, serve_up_first, serve_down_first, serve_gate_second, serve_up_second, serve_down_second, mixed)
```

```python
import functools

import jax
import jax.numpy as jnp
from jax import lax
from jax.experimental import pallas as pl
from jax.experimental.pallas import tpu as pltpu
from jax.sharding import PartitionSpec as P

MESH = pl.DeviceIdType.MESH


def gather_kernel(
    n_gr,
    n_fs,
    n_tp,
    gain_ref,
    gate_ref,
    up_ref,
    down_ref,
    gate_out,
    up_out,
    down_out,
    down_own,
    line_send,
    line_recv,
    pair_send,
    pair_recv,
    part_send,
    part_recv,
):
    g, f, t = lax.axis_index("gr"), lax.axis_index("fs"), lax.axis_index("tp")
    per = n_gr * n_fs // n_tp
    cols = down_ref.shape[1]
    first = lax.rem(t * per, n_fs)
    home = (t * per) // n_fs
    row = g * n_fs + f
    owner = row // per
    slot = lax.rem(row, per)

    width = gate_ref.shape[1]

    def place(ref, origin):
        if len(ref.shape) == 3:
            return ref.at[origin]
        return ref.at[:, pl.ds(pl.multiple_of(origin * width, 128), width)]

    gain = gain_ref[...]
    place(gate_out, row)[...] = (gain * gate_ref[...]).astype(jnp.bfloat16)
    place(up_out, row)[...] = (gain * up_ref[...]).astype(jnp.bfloat16)
    down_own[...] = down_ref[...].astype(jnp.bfloat16)

    @pl.when(owner == t)
    def _():
        down_out[slot, :, pl.ds(pl.multiple_of(t * cols, 128), cols)] = down_ref[...].astype(
            jnp.bfloat16
        )

    barrier = pltpu.get_barrier_semaphore()
    for dg in range(n_gr):
        for dt in range(n_tp):
            if dg or dt:
                pl.semaphore_signal(
                    barrier,
                    inc=1,
                    device_id=(lax.rem(g + dg, n_gr), f, lax.rem(t + dt, n_tp)),
                    device_id_type=MESH,
                )

    for near in (lax.rem(f + 1, n_fs), lax.rem(f + n_fs - 1, n_fs)):
        pl.semaphore_signal(barrier, inc=1, device_id=(g, near, t), device_id_type=MESH)
    pl.semaphore_wait(barrier, n_gr * n_tp + 1)

    outs = (gate_out, up_out)

    def held(o):
        return jnp.logical_and(o >= first, o < first + per)

    def block(m, o):
        if m < 2:
            return place(outs[m], g * n_fs + o)
        return down_out.at[o - first]

    def line(m, way, s):
        step = 1 if way == 0 else -1
        o = f - step * (s - 1)
        return pltpu.make_async_remote_copy(
            src_ref=block(m, o),
            dst_ref=block(m, o),
            send_sem=line_send.at[m, way, s],
            recv_sem=line_recv.at[m, way, s],
            device_id=(g, f + step, t),
            device_id_type=MESH,
        )

    def sends(m, way, s):
        step = 1 if way == 0 else -1
        o = f - step * (s - 1)
        fine = (f < n_fs - 1, o >= 0) if way == 0 else (f > 0, o <= n_fs - 1)
        ok = jnp.logical_and(*fine)
        return jnp.logical_and(ok, held(o)) if m == 2 else ok

    def gets(m, way, s):
        o = f - s if way == 0 else f + s
        ok = o >= 0 if way == 0 else o <= n_fs - 1
        return jnp.logical_and(ok, held(o)) if m == 2 else ok

    def landed(m, way, s):
        o = f - s if way == 0 else f + s
        return pltpu.make_async_remote_copy(
            src_ref=block(m, o),
            dst_ref=block(m, o),
            send_sem=line_send.at[m, way, s],
            recv_sem=line_recv.at[m, way, s],
            device_id=(g, f, t),
            device_id_type=MESH,
        )

    def pair(m, dg, o):
        return pltpu.make_async_remote_copy(
            src_ref=place(outs[m], g * n_fs + o),
            dst_ref=place(outs[m], g * n_fs + o),
            send_sem=pair_send.at[m, dg, o],
            recv_sem=pair_recv.at[m, dg, o],
            device_id=(lax.rem(g + dg, n_gr), f, t),
            device_id_type=MESH,
        )

    def pair_landed(m, dg, o):
        src = lax.rem(g - dg + n_gr, n_gr)
        return pltpu.make_async_remote_copy(
            src_ref=place(outs[m], src * n_fs + o),
            dst_ref=place(outs[m], src * n_fs + o),
            send_sem=pair_send.at[m, dg, o],
            recv_sem=pair_recv.at[m, dg, o],
            device_id=(src, f, t),
            device_id_type=MESH,
        )

    def part(dg):
        to = lax.rem(g + dg, n_gr)
        return pltpu.make_async_remote_copy(
            src_ref=down_own,
            dst_ref=down_out.at[slot, :, pl.ds(pl.multiple_of(t * cols, 128), cols)],
            send_sem=part_send.at[dg],
            recv_sem=part_recv.at[t],
            device_id=(to, f, owner),
            device_id_type=MESH,
        )

    def part_landed(src):
        return pltpu.make_async_remote_copy(
            src_ref=down_own,
            dst_ref=down_out.at[f - first, :, pl.ds(src * cols, cols)],
            send_sem=part_send.at[0],
            recv_sem=part_recv.at[src],
            device_id=(home, f, src),
            device_id_type=MESH,
        )

    for m in range(2):
        for way in range(2):

            @pl.when(sends(m, way, 1))
            def _(m=m, way=way):
                line(m, way, 1).start()

        for dg in range(1, n_gr):
            pair(m, dg, f).start()
    for dg in range(n_gr):
        if dg == 0:

            @pl.when(owner != t)
            def _():
                part(0).start()

        else:
            part(dg).start()

    @pl.when(held(f))
    def _():
        for src in range(n_tp):

            @pl.when(jnp.logical_or(home != g, t != src))
            def _(src=src):
                part_landed(src).wait_recv()

    for way in range(2):

        @pl.when(sends(2, way, 1))
        def _(way=way):
            line(2, way, 1).start()

    for s in range(1, n_fs):
        for m in range(3):
            for way in range(2):

                @pl.when(gets(m, way, s))
                def _(m=m, way=way, s=s):
                    landed(m, way, s).wait_recv()
                    if s < n_fs - 1:

                        @pl.when(sends(m, way, s + 1))
                        def _():
                            line(m, way, s + 1).start()

                    if m < 2:
                        o = f - s if way == 0 else f + s
                        for dg in range(1, n_gr):
                            pair(m, dg, o).start()

    for m in range(2):
        for dg in range(1, n_gr):
            for o in range(n_fs):
                pair_landed(m, dg, o).wait_recv()
                pair(m, dg, o).wait_send()
    for m in range(3):
        for way in range(2):
            for s in range(1, n_fs):

                @pl.when(sends(m, way, s))
                def _(m=m, way=way, s=s):
                    line(m, way, s).wait_send()

    for dg in range(n_gr):
        if dg == 0:

            @pl.when(owner != t)
            def _():
                part(0).wait_send()

        else:
            part(dg).wait_send()


def gather(sizes, call, gain, gate, up, down):
    n_gr, n_fs, n_tp = sizes
    per = n_gr * n_fs // n_tp
    rows, width = gate.shape
    wide = rows % 128 == 0
    whole = (width, n_gr * n_fs * rows) if wide else (n_gr * n_fs, width, rows)
    tall, cols = down.shape
    vmem = pl.BlockSpec(memory_space=pltpu.VMEM)
    dma = pltpu.SemaphoreType.DMA
    gate_all, up_all, down_all = pl.pallas_call(
        functools.partial(gather_kernel, n_gr, n_fs, n_tp),
        out_shape=(
            jax.ShapeDtypeStruct(whole, jnp.bfloat16),
            jax.ShapeDtypeStruct(whole, jnp.bfloat16),
            jax.ShapeDtypeStruct((per, tall, n_tp * cols), jnp.bfloat16),
        ),
        in_specs=[vmem] * 4,
        out_specs=(vmem,) * 3,
        scratch_shapes=[
            pltpu.VMEM((tall, cols), jnp.bfloat16),
            dma((3, 2, n_fs)),
            dma((3, 2, n_fs)),
            dma((2, n_gr, n_fs)),
            dma((2, n_gr, n_fs)),
            dma((n_gr,)),
            dma((n_tp,)),
        ],
        compiler_params=pltpu.CompilerParams(
            collective_id=call, has_side_effects=True, vmem_limit_bytes=32 * 2**20
        ),
        cost_estimate=pl.CostEstimate(
            flops=10**10, bytes_accessed=16 * 2**20, transcendentals=0
        ),
    )(gain[None, :], gate.T, up.T, down)

    def upright(a):
        return a.T if wide else a.transpose(0, 2, 1).reshape(n_gr * n_fs * rows, width)

    return (
        upright(gate_all),
        upright(up_all),
        down_all.reshape(per * tall, n_tp * cols),
    )


def normalize(rows):
    rows = rows.astype(jnp.float32)
    scale = lax.rsqrt(jnp.mean(rows * rows, axis=-1, keepdims=True) + 1e-06)
    return (rows * scale).astype(jnp.bfloat16)


def hidden_units(normed, w_gate, w_up):
    gate = jnp.dot(normed, w_gate, preferred_element_type=jnp.float32)
    upper = jnp.dot(normed, w_up, preferred_element_type=jnp.float32)
    return (jax.nn.silu(gate) * upper).astype(jnp.bfloat16)


def rounded_term(hidden, w_down):
    return jnp.dot(hidden, w_down, preferred_element_type=jnp.float32).astype(jnp.bfloat16)


def shards(
    sizes,
    prompt,
    gain_first,
    gate_first,
    up_first,
    down_first,
    gain_second,
    gate_second,
    up_second,
    down_second,
):
    gate_a, up_a, down_a = gather(sizes, 0, gain_first, gate_first, up_first, down_first)
    hidden_a = hidden_units(normalize(prompt), gate_a, up_a)
    term_a = rounded_term(hidden_a, down_a)
    term_a, gain_second = lax.optimization_barrier((term_a, gain_second))
    branch_a = lax.psum(term_a, "tp").astype(jnp.float32)
    gate_b, up_b, down_b = gather(sizes, 1, gain_second, gate_second, up_second, down_second)
    stream = prompt.astype(jnp.float32) + 0.5 * branch_a
    hidden_b = hidden_units(normalize(stream), gate_b, up_b)
    owned = hidden_b.shape[0] // lax.axis_size("tp")
    branch_b = lax.psum_scatter(
        rounded_term(hidden_b, down_b), "tp", scatter_dimension=0, tiled=True
    ).astype(jnp.float32)
    own_stream = lax.dynamic_slice_in_dim(stream, lax.axis_index("tp") * owned, owned, 0)
    mixed = (own_stream + 0.5 * branch_b).astype(jnp.bfloat16)
    return (gate_a, up_a, down_a, gate_b, up_b, down_b, mixed)


def solution(mesh):
    sizes = (mesh.shape["gr"], mesh.shape["fs"], mesh.shape["tp"])
    return jax.shard_map(
        functools.partial(shards, sizes),
        mesh=mesh,
        in_specs=(
            P(("gr", "fs"), None),
            P(("gr", "fs")),
            P(("gr", "fs"), "tp"),
            P(("gr", "fs"), "tp"),
            P(("gr", "fs"), "tp"),
            P(("gr", "fs")),
            P(("gr", "fs"), "tp"),
            P(("gr", "fs"), "tp"),
            P(("gr", "fs"), "tp"),
        ),
        out_specs=(
            P(None, "tp"),
            P(None, "tp"),
            P("tp", None),
            P(None, "tp"),
            P(None, "tp"),
            P("tp", None),
            P(("gr", "fs", "tp"), None),
        ),
        check_vma=False,
    )
```

```python
import functools

import jax
import jax.numpy as jnp
from jax import lax
from jax.experimental import pallas as pl
from jax.experimental.pallas import tpu as pltpu
from jax.sharding import PartitionSpec as P

MESH = pl.DeviceIdType.MESH


def gather_kernel(
    n_gr,
    n_fs,
    n_tp,
    gain_ref,
    gate_ref,
    up_ref,
    down_ref,
    gate_out,
    up_out,
    down_out,
    down_own,
    line_send,
    line_recv,
    pair_send,
    pair_recv,
    part_send,
    part_recv,
):
    g, f, t = lax.axis_index("gr"), lax.axis_index("fs"), lax.axis_index("tp")
    per = n_gr * n_fs // n_tp
    cols = down_ref.shape[1]
    first = lax.rem(t * per, n_fs)
    home = (t * per) // n_fs
    row = g * n_fs + f
    owner = row // per
    slot = lax.rem(row, per)

    width = gate_ref.shape[1]

    def place(ref, origin):
        if len(ref.shape) == 3:
            return ref.at[origin]
        return ref.at[:, pl.ds(pl.multiple_of(origin * width, 128), width)]

    gain = gain_ref[...]
    place(gate_out, row)[...] = (gain * gate_ref[...]).astype(jnp.bfloat16)
    place(up_out, row)[...] = (gain * up_ref[...]).astype(jnp.bfloat16)
    down_own[...] = down_ref[...].astype(jnp.bfloat16)

    @pl.when(owner == t)
    def _():
        down_out[slot, :, pl.ds(pl.multiple_of(t * cols, 128), cols)] = down_ref[...].astype(
            jnp.bfloat16
        )

    barrier = pltpu.get_barrier_semaphore()
    for dg in range(n_gr):
        for dt in range(n_tp):
            if dg or dt:
                pl.semaphore_signal(
                    barrier,
                    inc=1,
                    device_id=(lax.rem(g + dg, n_gr), f, lax.rem(t + dt, n_tp)),
                    device_id_type=MESH,
                )

    for near in (lax.rem(f + 1, n_fs), lax.rem(f + n_fs - 1, n_fs)):
        pl.semaphore_signal(barrier, inc=1, device_id=(g, near, t), device_id_type=MESH)
    pl.semaphore_wait(barrier, n_gr * n_tp + 1)

    outs = (gate_out, up_out)

    def held(o):
        return jnp.logical_and(o >= first, o < first + per)

    def block(m, o):
        if m < 2:
            return place(outs[m], g * n_fs + o)
        return down_out.at[o - first]

    def line(m, way, s):
        step = 1 if way == 0 else -1
        o = f - step * (s - 1)
        return pltpu.make_async_remote_copy(
            src_ref=block(m, o),
            dst_ref=block(m, o),
            send_sem=line_send.at[m, way, s],
            recv_sem=line_recv.at[m, way, s],
            device_id=(g, f + step, t),
            device_id_type=MESH,
        )

    def sends(m, way, s):
        step = 1 if way == 0 else -1
        o = f - step * (s - 1)
        fine = (f < n_fs - 1, o >= 0) if way == 0 else (f > 0, o <= n_fs - 1)
        ok = jnp.logical_and(*fine)
        return jnp.logical_and(ok, held(o)) if m == 2 else ok

    def gets(m, way, s):
        o = f - s if way == 0 else f + s
        ok = o >= 0 if way == 0 else o <= n_fs - 1
        return jnp.logical_and(ok, held(o)) if m == 2 else ok

    def landed(m, way, s):
        o = f - s if way == 0 else f + s
        return pltpu.make_async_remote_copy(
            src_ref=block(m, o),
            dst_ref=block(m, o),
            send_sem=line_send.at[m, way, s],
            recv_sem=line_recv.at[m, way, s],
            device_id=(g, f, t),
            device_id_type=MESH,
        )

    def pair(m, dg, o):
        return pltpu.make_async_remote_copy(
            src_ref=place(outs[m], g * n_fs + o),
            dst_ref=place(outs[m], g * n_fs + o),
            send_sem=pair_send.at[m, dg, o],
            recv_sem=pair_recv.at[m, dg, o],
            device_id=(lax.rem(g + dg, n_gr), f, t),
            device_id_type=MESH,
        )

    def pair_landed(m, dg, o):
        src = lax.rem(g - dg + n_gr, n_gr)
        return pltpu.make_async_remote_copy(
            src_ref=place(outs[m], src * n_fs + o),
            dst_ref=place(outs[m], src * n_fs + o),
            send_sem=pair_send.at[m, dg, o],
            recv_sem=pair_recv.at[m, dg, o],
            device_id=(src, f, t),
            device_id_type=MESH,
        )

    def part(dg):
        to = lax.rem(g + dg, n_gr)
        return pltpu.make_async_remote_copy(
            src_ref=down_own,
            dst_ref=down_out.at[slot, :, pl.ds(pl.multiple_of(t * cols, 128), cols)],
            send_sem=part_send.at[dg],
            recv_sem=part_recv.at[t],
            device_id=(to, f, owner),
            device_id_type=MESH,
        )

    def part_landed(src):
        return pltpu.make_async_remote_copy(
            src_ref=down_own,
            dst_ref=down_out.at[f - first, :, pl.ds(src * cols, cols)],
            send_sem=part_send.at[0],
            recv_sem=part_recv.at[src],
            device_id=(home, f, src),
            device_id_type=MESH,
        )

    for m in range(2):
        for way in range(2):

            @pl.when(sends(m, way, 1))
            def _(m=m, way=way):
                line(m, way, 1).start()

        for dg in range(1, n_gr):
            pair(m, dg, f).start()
    for dg in range(n_gr):
        if dg == 0:

            @pl.when(owner != t)
            def _():
                part(0).start()

        else:
            part(dg).start()

    @pl.when(held(f))
    def _():
        for src in range(n_tp):

            @pl.when(jnp.logical_or(home != g, t != src))
            def _(src=src):
                part_landed(src).wait_recv()

    for way in range(2):

        @pl.when(sends(2, way, 1))
        def _(way=way):
            line(2, way, 1).start()

    for s in range(1, n_fs):
        for m in range(3):
            for way in range(2):

                @pl.when(gets(m, way, s))
                def _(m=m, way=way, s=s):
                    landed(m, way, s).wait_recv()
                    if s < n_fs - 1:

                        @pl.when(sends(m, way, s + 1))
                        def _():
                            line(m, way, s + 1).start()

                    if m < 2:
                        o = f - s if way == 0 else f + s
                        for dg in range(1, n_gr):
                            pair(m, dg, o).start()

    for m in range(2):
        for dg in range(1, n_gr):
            for o in range(n_fs):
                pair_landed(m, dg, o).wait_recv()
                pair(m, dg, o).wait_send()
    for m in range(3):
        for way in range(2):
            for s in range(1, n_fs):

                @pl.when(sends(m, way, s))
                def _(m=m, way=way, s=s):
                    line(m, way, s).wait_send()

    for dg in range(n_gr):
        if dg == 0:

            @pl.when(owner != t)
            def _():
                part(0).wait_send()

        else:
            part(dg).wait_send()


def gather(sizes, call, gain, gate, up, down):
    n_gr, n_fs, n_tp = sizes
    per = n_gr * n_fs // n_tp
    rows, width = gate.shape
    wide = rows % 128 == 0
    whole = (width, n_gr * n_fs * rows) if wide else (n_gr * n_fs, width, rows)
    tall, cols = down.shape
    vmem = pl.BlockSpec(memory_space=pltpu.VMEM)
    dma = pltpu.SemaphoreType.DMA
    gate_all, up_all, down_all = pl.pallas_call(
        functools.partial(gather_kernel, n_gr, n_fs, n_tp),
        out_shape=(
            jax.ShapeDtypeStruct(whole, jnp.bfloat16),
            jax.ShapeDtypeStruct(whole, jnp.bfloat16),
            jax.ShapeDtypeStruct((per, tall, n_tp * cols), jnp.bfloat16),
        ),
        in_specs=[vmem] * 4,
        out_specs=(vmem,) * 3,
        scratch_shapes=[
            pltpu.VMEM((tall, cols), jnp.bfloat16),
            dma((3, 2, n_fs)),
            dma((3, 2, n_fs)),
            dma((2, n_gr, n_fs)),
            dma((2, n_gr, n_fs)),
            dma((n_gr,)),
            dma((n_tp,)),
        ],
        compiler_params=pltpu.CompilerParams(
            collective_id=call, has_side_effects=True, vmem_limit_bytes=32 * 2**20
        ),
        cost_estimate=pl.CostEstimate(
            flops=10**10, bytes_accessed=16 * 2**20, transcendentals=0
        ),
    )(gain[None, :], gate.T, up.T, down)

    def upright(a):
        return a.T if wide else a.transpose(0, 2, 1).reshape(n_gr * n_fs * rows, width)

    return (
        upright(gate_all),
        upright(up_all),
        down_all.reshape(per * tall, n_tp * cols),
    )


def fused_kernel(
    n_gr,
    n_fs,
    n_tp,
    prompt_ref,
    gain_a,
    gate_a,
    up_a,
    down_a,
    gain_b,
    gate_b,
    up_b,
    down_b,
    gate_out_a,
    up_out_a,
    down_out_a,
    gate_out_b,
    up_out_b,
    down_out_b,
    mixed_ref,
    down_own,
    normed,
    normed_all,
    hidden,
    parts,
    parts_in,
    stream,
    line_send,
    line_recv,
    pair_send,
    pair_recv,
    part_send,
    part_recv,
    sum_send,
    sum_recv,
    row_send,
    row_recv,
):
    g, f, t = lax.axis_index("gr"), lax.axis_index("fs"), lax.axis_index("tp")
    per = n_gr * n_fs // n_tp
    cols = down_a.shape[1]
    width = gate_a.shape[1]
    first = lax.rem(t * per, n_fs)
    home = (t * per) // n_fs
    row = g * n_fs + f
    owner = row // per
    slot = lax.rem(row, per)
    outs = ((gate_out_a, up_out_a, down_out_a), (gate_out_b, up_out_b, down_out_b))

    def place(ref, origin):
        return ref.at[:, pl.ds(pl.multiple_of(origin * width, 128), width)]

    for n, (gain, gate, up, down) in enumerate(
        ((gain_a, gate_a, up_a, down_a), (gain_b, gate_b, up_b, down_b))
    ):
        place(outs[n][0], row)[...] = (gain[...] * gate[...]).astype(jnp.bfloat16)
        place(outs[n][1], row)[...] = (gain[...] * up[...]).astype(jnp.bfloat16)
        down_own[n] = down[...].astype(jnp.bfloat16)

        @pl.when(owner == t)
        def _(n=n, down=down):
            outs[n][2][slot, :, pl.ds(pl.multiple_of(t * cols, 128), cols)] = down[...].astype(
                jnp.bfloat16
            )

    barrier = pltpu.get_barrier_semaphore()
    for dg in range(n_gr):
        for dt in range(n_tp):
            if dg or dt:
                pl.semaphore_signal(
                    barrier,
                    inc=1,
                    device_id=(lax.rem(g + dg, n_gr), f, lax.rem(t + dt, n_tp)),
                    device_id_type=MESH,
                )
    for near in (lax.rem(f + 1, n_fs), lax.rem(f + n_fs - 1, n_fs)):
        pl.semaphore_signal(barrier, inc=1, device_id=(g, near, t), device_id_type=MESH)
    pl.semaphore_wait(barrier, n_gr * n_tp + 1)

    def held(o):
        return jnp.logical_and(o >= first, o < first + per)

    def remote(src, dst, send, recv, to):
        return pltpu.make_async_remote_copy(
            src_ref=src,
            dst_ref=dst,
            send_sem=send,
            recv_sem=recv,
            device_id=to,
            device_id_type=MESH,
        )

    def block(n, m, o):
        if m < 2:
            return place(outs[n][m], g * n_fs + o)
        return outs[n][2].at[o - first]

    def line(n, m, way, s):
        step = 1 if way == 0 else -1
        o = f - step * (s - 1)
        sems = line_send.at[n, m, way, s], line_recv.at[n, m, way, s]
        return remote(block(n, m, o), block(n, m, o), *sems, (g, f + step, t))

    def sends(m, way, s):
        step = 1 if way == 0 else -1
        o = f - step * (s - 1)
        fine = (f < n_fs - 1, o >= 0) if way == 0 else (f > 0, o <= n_fs - 1)
        ok = jnp.logical_and(*fine)
        return jnp.logical_and(ok, held(o)) if m == 2 else ok

    def gets(m, way, s):
        o = f - s if way == 0 else f + s
        ok = o >= 0 if way == 0 else o <= n_fs - 1
        return jnp.logical_and(ok, held(o)) if m == 2 else ok

    def landed(n, m, way, s):
        o = f - s if way == 0 else f + s
        sems = line_send.at[n, m, way, s], line_recv.at[n, m, way, s]
        return remote(block(n, m, o), block(n, m, o), *sems, (g, f, t))

    def pair(n, m, dg, o):
        spot = place(outs[n][m], g * n_fs + o)
        sems = pair_send.at[n, m, dg, o], pair_recv.at[n, m, dg, o]
        return remote(spot, spot, *sems, (lax.rem(g + dg, n_gr), f, t))

    def pair_landed(n, m, dg, o):
        src = lax.rem(g - dg + n_gr, n_gr)
        spot = place(outs[n][m], src * n_fs + o)
        sems = pair_send.at[n, m, dg, o], pair_recv.at[n, m, dg, o]
        return remote(spot, spot, *sems, (src, f, t))

    def part(n, dg):
        return remote(
            down_own.at[n],
            outs[n][2].at[slot, :, pl.ds(pl.multiple_of(t * cols, 128), cols)],
            part_send.at[n, dg],
            part_recv.at[n, t],
            (lax.rem(g + dg, n_gr), f, owner),
        )

    def part_landed(n, src):
        return remote(
            down_own.at[n],
            outs[n][2].at[f - first, :, pl.ds(src * cols, cols)],
            part_send.at[n, 0],
            part_recv.at[n, src],
            (home, f, src),
        )

    def start_own(n):
        for m in range(2):
            for way in range(2):

                @pl.when(sends(m, way, 1))
                def _(m=m, way=way):
                    line(n, m, way, 1).start()

            for dg in range(1, n_gr):
                pair(n, m, dg, f).start()
        for dg in range(n_gr):
            if dg == 0:

                @pl.when(owner != t)
                def _():
                    part(n, 0).start()

            else:
                part(n, dg).start()

    def start_down(n):
        @pl.when(held(f))
        def _():
            for src in range(n_tp):

                @pl.when(jnp.logical_or(home != g, t != src))
                def _(src=src):
                    part_landed(n, src).wait_recv()

        for way in range(2):

            @pl.when(sends(2, way, 1))
            def _(way=way):
                line(n, 2, way, 1).start()

    def forward(n, m, s):
        for way in range(2):

            @pl.when(gets(m, way, s))
            def _(way=way):
                landed(n, m, way, s).wait_recv()
                if s < n_fs - 1:

                    @pl.when(sends(m, way, s + 1))
                    def _():
                        line(n, m, way, s + 1).start()

                if m < 2:
                    o = f - s if way == 0 else f + s
                    for dg in range(1, n_gr):
                        pair(n, m, dg, o).start()

    def pairs_in(n):
        for m in range(2):
            for dg in range(1, n_gr):
                for o in range(n_fs):
                    pair_landed(n, m, dg, o).wait_recv()

    def drain(n):
        for m in range(2):
            for dg in range(1, n_gr):
                for o in range(n_fs):
                    pair(n, m, dg, o).wait_send()
        for m in range(3):
            for way in range(2):
                for s in range(1, n_fs):

                    @pl.when(sends(m, way, s))
                    def _(m=m, way=way, s=s):
                        line(n, m, way, s).wait_send()

        for dg in range(n_gr):
            if dg == 0:

                @pl.when(owner != t)
                def _():
                    part(n, 0).wait_send()

            else:
                part(n, dg).wait_send()

    owned, depth = prompt_ref.shape[1], prompt_ref.shape[2]
    across = (((1,), (1,)), ((), ()))

    def unit(rows):
        return rows * lax.rsqrt(jnp.mean(rows * rows, axis=-1, keepdims=True) + 1e-06)

    def hide(n, source):
        @pl.loop(0, n_tp // 2)
        def _(i):
            rows = source[pl.ds(2 * i, 2)].reshape(2 * owned, depth)
            gate = lax.dot_general(
                rows, outs[n][0][...], across, preferred_element_type=jnp.float32
            )
            upper = lax.dot_general(
                rows, outs[n][1][...], across, preferred_element_type=jnp.float32
            )
            units = (jax.nn.silu(gate) * upper).astype(jnp.bfloat16)
            hidden[pl.ds(2 * i, 2)] = units.reshape(2, owned, units.shape[1])

    def share(n, i):
        to = lax.rem(t + 1 + i, n_tp)
        return remote(
            parts.at[n, to],
            parts_in.at[n, i],
            sum_send.at[n, i],
            sum_recv.at[n, i],
            (g, f, to),
        )

    def spread(n):
        tall = outs[n][2].shape[1]

        @pl.loop(0, n_tp)
        def _(i):
            to = lax.rem(t + 1 + i, n_tp)
            units = hidden[to]
            term = jnp.zeros((owned, depth), jnp.float32)
            for k in range(per):
                term += jnp.dot(
                    units[:, k * tall : (k + 1) * tall],
                    outs[n][2][k],
                    preferred_element_type=jnp.float32,
                )
            parts[n, to] = term.astype(jnp.bfloat16)

            @pl.when(i > 0)
            def _():
                share(n, i - 1).start()

    def collect(n):
        total = parts[n, t].astype(jnp.float32)
        for i in range(n_tp - 1):
            share(n, i).wait_recv()
            total += parts_in[n, i].astype(jnp.float32)
        return total

    def give(i):
        to = lax.rem(t + 1 + i, n_tp)
        return remote(
            normed_all.at[t], normed_all.at[t], row_send.at[i], row_recv.at[i], (g, f, to)
        )

    def given(i):
        src = lax.rem(t - 1 - i + n_tp, n_tp)
        return remote(
            normed_all.at[src], normed_all.at[src], row_send.at[i], row_recv.at[i], (g, f, src)
        )

    start_own(0)

    @pl.loop(0, n_tp)
    def _(i):
        normed[i] = unit(prompt_ref[i].astype(jnp.float32)).astype(jnp.bfloat16)

    start_down(0)
    for m in range(3):
        forward(0, m, 1)
    start_own(1)
    for s in range(2, n_fs):
        for m in range(3):
            forward(0, m, s)
    start_down(1)
    pairs_in(0)
    hide(0, normed)
    for m in range(3):
        forward(1, m, 1)
    spread(0)
    for s in range(2, n_fs - 1):
        for m in range(3):
            forward(1, m, s)
    stream[...] = prompt_ref[t].astype(jnp.float32) + 0.5 * collect(0)
    normed_all[t] = unit(stream[...]).astype(jnp.bfloat16)
    for m in range(2):
        forward(1, m, n_fs - 1)
    for i in range(n_tp - 1):
        give(i).start()
    for i in range(n_tp - 1):
        given(i).wait_recv()
    pairs_in(1)
    hide(1, normed_all)
    forward(1, 2, n_fs - 1)
    spread(1)
    drain(0)
    drain(1)
    mixed_ref[...] = (stream[...] + 0.5 * collect(1)).astype(jnp.bfloat16)
    for i in range(n_tp - 1):
        give(i).wait_send()
        share(0, i).wait_send()
        share(1, i).wait_send()


def fused(sizes, prompt, *weights):
    n_gr, n_fs, n_tp = sizes
    per = n_gr * n_fs // n_tp
    tokens, depth = prompt.shape
    owned = tokens // n_tp
    rows, width = weights[1].shape
    tall, cols = weights[3].shape
    vmem = pl.BlockSpec(memory_space=pltpu.VMEM)
    dma = pltpu.SemaphoreType.DMA
    across = jax.ShapeDtypeStruct((width, n_gr * n_fs * rows), jnp.bfloat16)
    down = jax.ShapeDtypeStruct((per, tall, n_tp * cols), jnp.bfloat16)
    operands = [prompt.reshape(n_tp, owned, depth)]
    for n in range(2):
        gain, gate, up, tall_block = weights[4 * n : 4 * n + 4]
        operands += [gain[None, :], gate.T, up.T, tall_block]
    *served, mixed = pl.pallas_call(
        functools.partial(fused_kernel, n_gr, n_fs, n_tp),
        out_shape=(across, across, down) * 2
        + (jax.ShapeDtypeStruct((owned, depth), jnp.bfloat16),),
        in_specs=[vmem] * 9,
        out_specs=(vmem,) * 7,
        scratch_shapes=[
            pltpu.VMEM((2, tall, cols), jnp.bfloat16),
            pltpu.VMEM((n_tp, owned, depth), jnp.bfloat16),
            pltpu.VMEM((n_tp, owned, depth), jnp.bfloat16),
            pltpu.VMEM((n_tp, owned, width), jnp.bfloat16),
            pltpu.VMEM((2, n_tp, owned, depth), jnp.bfloat16),
            pltpu.VMEM((2, n_tp - 1, owned, depth), jnp.bfloat16),
            pltpu.VMEM((owned, depth), jnp.float32),
            dma((2, 3, 2, n_fs)),
            dma((2, 3, 2, n_fs)),
            dma((2, 2, n_gr, n_fs)),
            dma((2, 2, n_gr, n_fs)),
            dma((2, n_gr)),
            dma((2, n_tp)),
            dma((2, n_tp - 1)),
            dma((2, n_tp - 1)),
            dma((n_tp - 1,)),
            dma((n_tp - 1,)),
        ],
        compiler_params=pltpu.CompilerParams(
            collective_id=2, has_side_effects=True, vmem_limit_bytes=60 * 2**20
        ),
    )(*operands)
    gate_a, up_a, down_a, gate_b, up_b, down_b = served

    def flat(a):
        return a.reshape(per * tall, n_tp * cols)

    return (gate_a.T, up_a.T, flat(down_a), gate_b.T, up_b.T, flat(down_b), mixed)


def normalize(rows):
    rows = rows.astype(jnp.float32)
    scale = lax.rsqrt(jnp.mean(rows * rows, axis=-1, keepdims=True) + 1e-06)
    return (rows * scale).astype(jnp.bfloat16)


def hidden_units(normed, w_gate, w_up):
    gate = jnp.dot(normed, w_gate, preferred_element_type=jnp.float32)
    upper = jnp.dot(normed, w_up, preferred_element_type=jnp.float32)
    return (jax.nn.silu(gate) * upper).astype(jnp.bfloat16)


def rounded_term(hidden, w_down):
    return jnp.dot(hidden, w_down, preferred_element_type=jnp.float32).astype(jnp.bfloat16)


def shards(
    sizes,
    prompt,
    gain_first,
    gate_first,
    up_first,
    down_first,
    gain_second,
    gate_second,
    up_second,
    down_second,
):
    if gate_first.shape[0] % 128 == 0 and sizes[2] % 2 == 0:
        return fused(
            sizes,
            prompt,
            gain_first,
            gate_first,
            up_first,
            down_first,
            gain_second,
            gate_second,
            up_second,
            down_second,
        )
    gate_a, up_a, down_a = gather(sizes, 0, gain_first, gate_first, up_first, down_first)
    hidden_a = hidden_units(normalize(prompt), gate_a, up_a)
    term_a = rounded_term(hidden_a, down_a)
    term_a, gain_second = lax.optimization_barrier((term_a, gain_second))
    branch_a = lax.psum(term_a, "tp").astype(jnp.float32)
    gate_b, up_b, down_b = gather(sizes, 1, gain_second, gate_second, up_second, down_second)
    stream = prompt.astype(jnp.float32) + 0.5 * branch_a
    hidden_b = hidden_units(normalize(stream), gate_b, up_b)
    owned = hidden_b.shape[0] // lax.axis_size("tp")
    branch_b = lax.psum_scatter(
        rounded_term(hidden_b, down_b), "tp", scatter_dimension=0, tiled=True
    ).astype(jnp.float32)
    own_stream = lax.dynamic_slice_in_dim(stream, lax.axis_index("tp") * owned, owned, 0)
    mixed = (own_stream + 0.5 * branch_b).astype(jnp.bfloat16)
    return (gate_a, up_a, down_a, gate_b, up_b, down_b, mixed)


def solution(mesh):
    sizes = (mesh.shape["gr"], mesh.shape["fs"], mesh.shape["tp"])
    return jax.shard_map(
        functools.partial(shards, sizes),
        mesh=mesh,
        in_specs=(
            P(("gr", "fs"), None),
            P(("gr", "fs")),
            P(("gr", "fs"), "tp"),
            P(("gr", "fs"), "tp"),
            P(("gr", "fs"), "tp"),
            P(("gr", "fs")),
            P(("gr", "fs"), "tp"),
            P(("gr", "fs"), "tp"),
            P(("gr", "fs"), "tp"),
        ),
        out_specs=(
            P(None, "tp"),
            P(None, "tp"),
            P("tp", None),
            P(None, "tp"),
            P(None, "tp"),
            P("tp", None),
            P(("gr", "fs", "tp"), None),
        ),
        check_vma=False,
    )
```

```python
import functools

import jax
import jax.numpy as jnp
from jax import lax
from jax.experimental import pallas as pl
from jax.experimental.pallas import tpu as pltpu
from jax.sharding import PartitionSpec as P

MESH = pl.DeviceIdType.MESH


def gather_kernel(
    n_gr,
    n_fs,
    n_tp,
    gain_ref,
    gate_ref,
    up_ref,
    down_ref,
    gate_out,
    up_out,
    down_out,
    down_own,
    line_send,
    line_recv,
    pair_send,
    pair_recv,
    part_send,
    part_recv,
):
    g, f, t = lax.axis_index("gr"), lax.axis_index("fs"), lax.axis_index("tp")
    per = n_gr * n_fs // n_tp
    cols = down_ref.shape[1]
    first = lax.rem(t * per, n_fs)
    home = (t * per) // n_fs
    row = g * n_fs + f
    owner = row // per
    slot = lax.rem(row, per)

    width = gate_ref.shape[1]

    def place(ref, origin):
        if len(ref.shape) == 3:
            return ref.at[origin]
        return ref.at[:, pl.ds(pl.multiple_of(origin * width, 128), width)]

    gain = gain_ref[...]
    place(gate_out, row)[...] = (gain * gate_ref[...]).astype(jnp.bfloat16)
    place(up_out, row)[...] = (gain * up_ref[...]).astype(jnp.bfloat16)
    down_own[...] = down_ref[...].astype(jnp.bfloat16)

    @pl.when(owner == t)
    def _():
        down_out[slot, :, pl.ds(pl.multiple_of(t * cols, 128), cols)] = down_ref[...].astype(
            jnp.bfloat16
        )

    barrier = pltpu.get_barrier_semaphore()
    for dg in range(n_gr):
        for dt in range(n_tp):
            if dg or dt:
                pl.semaphore_signal(
                    barrier,
                    inc=1,
                    device_id=(lax.rem(g + dg, n_gr), f, lax.rem(t + dt, n_tp)),
                    device_id_type=MESH,
                )

    for near in (lax.rem(f + 1, n_fs), lax.rem(f + n_fs - 1, n_fs)):
        pl.semaphore_signal(barrier, inc=1, device_id=(g, near, t), device_id_type=MESH)
    pl.semaphore_wait(barrier, n_gr * n_tp + 1)

    outs = (gate_out, up_out)

    def held(o):
        return jnp.logical_and(o >= first, o < first + per)

    def block(m, o):
        if m < 2:
            return place(outs[m], g * n_fs + o)
        return down_out.at[o - first]

    def line(m, way, s):
        step = 1 if way == 0 else -1
        o = f - step * (s - 1)
        return pltpu.make_async_remote_copy(
            src_ref=block(m, o),
            dst_ref=block(m, o),
            send_sem=line_send.at[m, way, s],
            recv_sem=line_recv.at[m, way, s],
            device_id=(g, f + step, t),
            device_id_type=MESH,
        )

    def sends(m, way, s):
        step = 1 if way == 0 else -1
        o = f - step * (s - 1)
        fine = (f < n_fs - 1, o >= 0) if way == 0 else (f > 0, o <= n_fs - 1)
        ok = jnp.logical_and(*fine)
        return jnp.logical_and(ok, held(o)) if m == 2 else ok

    def gets(m, way, s):
        o = f - s if way == 0 else f + s
        ok = o >= 0 if way == 0 else o <= n_fs - 1
        return jnp.logical_and(ok, held(o)) if m == 2 else ok

    def landed(m, way, s):
        o = f - s if way == 0 else f + s
        return pltpu.make_async_remote_copy(
            src_ref=block(m, o),
            dst_ref=block(m, o),
            send_sem=line_send.at[m, way, s],
            recv_sem=line_recv.at[m, way, s],
            device_id=(g, f, t),
            device_id_type=MESH,
        )

    def pair(m, dg, o):
        return pltpu.make_async_remote_copy(
            src_ref=place(outs[m], g * n_fs + o),
            dst_ref=place(outs[m], g * n_fs + o),
            send_sem=pair_send.at[m, dg, o],
            recv_sem=pair_recv.at[m, dg, o],
            device_id=(lax.rem(g + dg, n_gr), f, t),
            device_id_type=MESH,
        )

    def pair_landed(m, dg, o):
        src = lax.rem(g - dg + n_gr, n_gr)
        return pltpu.make_async_remote_copy(
            src_ref=place(outs[m], src * n_fs + o),
            dst_ref=place(outs[m], src * n_fs + o),
            send_sem=pair_send.at[m, dg, o],
            recv_sem=pair_recv.at[m, dg, o],
            device_id=(src, f, t),
            device_id_type=MESH,
        )

    def part(dg):
        to = lax.rem(g + dg, n_gr)
        return pltpu.make_async_remote_copy(
            src_ref=down_own,
            dst_ref=down_out.at[slot, :, pl.ds(pl.multiple_of(t * cols, 128), cols)],
            send_sem=part_send.at[dg],
            recv_sem=part_recv.at[t],
            device_id=(to, f, owner),
            device_id_type=MESH,
        )

    def part_landed(src):
        return pltpu.make_async_remote_copy(
            src_ref=down_own,
            dst_ref=down_out.at[f - first, :, pl.ds(src * cols, cols)],
            send_sem=part_send.at[0],
            recv_sem=part_recv.at[src],
            device_id=(home, f, src),
            device_id_type=MESH,
        )

    for m in range(2):
        for way in range(2):

            @pl.when(sends(m, way, 1))
            def _(m=m, way=way):
                line(m, way, 1).start()

        for dg in range(1, n_gr):
            pair(m, dg, f).start()
    for dg in range(n_gr):
        if dg == 0:

            @pl.when(owner != t)
            def _():
                part(0).start()

        else:
            part(dg).start()

    @pl.when(held(f))
    def _():
        for src in range(n_tp):

            @pl.when(jnp.logical_or(home != g, t != src))
            def _(src=src):
                part_landed(src).wait_recv()

    for way in range(2):

        @pl.when(sends(2, way, 1))
        def _(way=way):
            line(2, way, 1).start()

    for s in range(1, n_fs):
        for m in range(3):
            for way in range(2):

                @pl.when(gets(m, way, s))
                def _(m=m, way=way, s=s):
                    landed(m, way, s).wait_recv()
                    if s < n_fs - 1:

                        @pl.when(sends(m, way, s + 1))
                        def _():
                            line(m, way, s + 1).start()

                    if m < 2:
                        o = f - s if way == 0 else f + s
                        for dg in range(1, n_gr):
                            pair(m, dg, o).start()

    for m in range(2):
        for dg in range(1, n_gr):
            for o in range(n_fs):
                pair_landed(m, dg, o).wait_recv()
                pair(m, dg, o).wait_send()
    for m in range(3):
        for way in range(2):
            for s in range(1, n_fs):

                @pl.when(sends(m, way, s))
                def _(m=m, way=way, s=s):
                    line(m, way, s).wait_send()

    for dg in range(n_gr):
        if dg == 0:

            @pl.when(owner != t)
            def _():
                part(0).wait_send()

        else:
            part(dg).wait_send()


def gather(sizes, call, gain, gate, up, down):
    n_gr, n_fs, n_tp = sizes
    per = n_gr * n_fs // n_tp
    rows, width = gate.shape
    wide = rows % 128 == 0
    whole = (width, n_gr * n_fs * rows) if wide else (n_gr * n_fs, width, rows)
    tall, cols = down.shape
    vmem = pl.BlockSpec(memory_space=pltpu.VMEM)
    dma = pltpu.SemaphoreType.DMA
    gate_all, up_all, down_all = pl.pallas_call(
        functools.partial(gather_kernel, n_gr, n_fs, n_tp),
        out_shape=(
            jax.ShapeDtypeStruct(whole, jnp.bfloat16),
            jax.ShapeDtypeStruct(whole, jnp.bfloat16),
            jax.ShapeDtypeStruct((per, tall, n_tp * cols), jnp.bfloat16),
        ),
        in_specs=[vmem] * 4,
        out_specs=(vmem,) * 3,
        scratch_shapes=[
            pltpu.VMEM((tall, cols), jnp.bfloat16),
            dma((3, 2, n_fs)),
            dma((3, 2, n_fs)),
            dma((2, n_gr, n_fs)),
            dma((2, n_gr, n_fs)),
            dma((n_gr,)),
            dma((n_tp,)),
        ],
        compiler_params=pltpu.CompilerParams(
            collective_id=call, has_side_effects=True, vmem_limit_bytes=32 * 2**20
        ),
        cost_estimate=pl.CostEstimate(
            flops=10**10, bytes_accessed=16 * 2**20, transcendentals=0
        ),
    )(gain[None, :], gate.T, up.T, down)

    def upright(a):
        return a.T if wide else a.transpose(0, 2, 1).reshape(n_gr * n_fs * rows, width)

    return (
        upright(gate_all),
        upright(up_all),
        down_all.reshape(per * tall, n_tp * cols),
    )


def fused_kernel(
    n_gr,
    n_fs,
    n_tp,
    prompt_ref,
    gain_a,
    gate_a,
    up_a,
    down_a,
    gain_b,
    gate_b,
    up_b,
    down_b,
    gate_out_a,
    up_out_a,
    down_out_a,
    gate_out_b,
    up_out_b,
    down_out_b,
    mixed_ref,
    down_own,
    normed,
    normed_all,
    hidden,
    parts,
    mate_in,
    sums,
    parts_in,
    kept,
    stream,
    line_send,
    line_recv,
    pair_send,
    pair_recv,
    part_send,
    part_recv,
    mate_send,
    mate_recv,
    sum_send,
    sum_recv,
    row_send,
    row_recv,
):
    g, f, t = lax.axis_index("gr"), lax.axis_index("fs"), lax.axis_index("tp")
    per = n_gr * n_fs // n_tp
    cols = down_a.shape[1]
    width = gate_a.shape[1]
    first = lax.rem(t * per, n_fs)
    home = (t * per) // n_fs
    row = g * n_fs + f
    owner = row // per
    slot = lax.rem(row, per)
    half = n_tp * cols // n_gr
    lane = t * n_gr // n_tp
    outs = ((gate_out_a, up_out_a, down_out_a), (gate_out_b, up_out_b, down_out_b))

    def halved(n):
        return n == 1

    def place(ref, origin):
        return ref.at[:, pl.ds(pl.multiple_of(origin * width, 128), width)]

    for n, (gain, gate, up, down) in enumerate(
        ((gain_a, gate_a, up_a, down_a), (gain_b, gate_b, up_b, down_b))
    ):
        place(outs[n][0], row)[...] = (gain[...] * gate[...]).astype(jnp.bfloat16)
        place(outs[n][1], row)[...] = (gain[...] * up[...]).astype(jnp.bfloat16)
        down_own[n] = down[...].astype(jnp.bfloat16)

        @pl.when(jnp.logical_and(owner == t, lane == g) if halved(n) else owner == t)
        def _(n=n, down=down):
            outs[n][2][slot, :, pl.ds(pl.multiple_of(t * cols, 128), cols)] = down[...].astype(
                jnp.bfloat16
            )

    barrier = pltpu.get_barrier_semaphore()
    for dg in range(n_gr):
        for dt in range(n_tp):
            if dg or dt:
                pl.semaphore_signal(
                    barrier,
                    inc=1,
                    device_id=(lax.rem(g + dg, n_gr), f, lax.rem(t + dt, n_tp)),
                    device_id_type=MESH,
                )
    for near in (lax.rem(f + 1, n_fs), lax.rem(f + n_fs - 1, n_fs)):
        pl.semaphore_signal(barrier, inc=1, device_id=(g, near, t), device_id_type=MESH)
    pl.semaphore_wait(barrier, n_gr * n_tp + 1)

    def held(o):
        return jnp.logical_and(o >= first, o < first + per)

    def remote(src, dst, send, recv, to):
        return pltpu.make_async_remote_copy(
            src_ref=src,
            dst_ref=dst,
            send_sem=send,
            recv_sem=recv,
            device_id=to,
            device_id_type=MESH,
        )

    def block(n, m, o):
        if m < 2:
            return place(outs[n][m], g * n_fs + o)
        if halved(n):
            return share_of(n, o, g)
        return outs[n][2].at[o - first]

    def share_of(n, o, column):
        return outs[n][2].at[o - first, :, pl.ds(pl.multiple_of(column * half, 128), half)]

    def line(n, m, way, s):
        step = 1 if way == 0 else -1
        o = f - step * (s - 1)
        sems = line_send.at[n, m, way, s], line_recv.at[n, m, way, s]
        return remote(block(n, m, o), block(n, m, o), *sems, (g, f + step, t))

    def sends(m, way, s):
        step = 1 if way == 0 else -1
        o = f - step * (s - 1)
        fine = (f < n_fs - 1, o >= 0) if way == 0 else (f > 0, o <= n_fs - 1)
        ok = jnp.logical_and(*fine)
        return jnp.logical_and(ok, held(o)) if m == 2 else ok

    def gets(m, way, s):
        o = f - s if way == 0 else f + s
        ok = o >= 0 if way == 0 else o <= n_fs - 1
        return jnp.logical_and(ok, held(o)) if m == 2 else ok

    def landed(n, m, way, s):
        o = f - s if way == 0 else f + s
        sems = line_send.at[n, m, way, s], line_recv.at[n, m, way, s]
        return remote(block(n, m, o), block(n, m, o), *sems, (g, f, t))

    def pair(n, m, dg, o):
        spot = share_of(n, o, g) if m == 2 else place(outs[n][m], g * n_fs + o)
        sems = pair_send.at[n, m, dg, o], pair_recv.at[n, m, dg, o]
        return remote(spot, spot, *sems, (lax.rem(g + dg, n_gr), f, t))

    def pair_landed(n, m, dg, o):
        src = lax.rem(g - dg + n_gr, n_gr)
        spot = share_of(n, o, src) if m == 2 else place(outs[n][m], src * n_fs + o)
        sems = pair_send.at[n, m, dg, o], pair_recv.at[n, m, dg, o]
        return remote(spot, spot, *sems, (src, f, t))

    def part(n, dg):
        return remote(
            down_own.at[n],
            outs[n][2].at[slot, :, pl.ds(pl.multiple_of(t * cols, 128), cols)],
            part_send.at[n, dg],
            part_recv.at[n, t],
            (lane if halved(n) else lax.rem(g + dg, n_gr), f, owner),
        )

    def part_landed(n, src):
        return remote(
            down_own.at[n],
            outs[n][2].at[f - first, :, pl.ds(src * cols, cols)],
            part_send.at[n, 0],
            part_recv.at[n, src],
            (home, f, src),
        )

    def start_own(n):
        for m in range(2):
            for way in range(2):

                @pl.when(sends(m, way, 1))
                def _(m=m, way=way):
                    line(n, m, way, 1).start()

            for dg in range(1, n_gr):
                pair(n, m, dg, f).start()
        for dg in range(n_gr):
            if halved(n):
                if dg == 0:

                    @pl.when(jnp.logical_or(owner != t, lane != g))
                    def _():
                        part(n, 0).start()

            elif dg == 0:

                @pl.when(owner != t)
                def _():
                    part(n, 0).start()

            else:
                part(n, dg).start()

    def start_down(n):
        @pl.when(held(f))
        def _():
            for src in range(n_tp):

                away = jnp.logical_or(home != g, t != src)
                if halved(n):
                    away = jnp.logical_and(away, g == src * n_gr // n_tp)

                @pl.when(away)
                def _(src=src):
                    part_landed(n, src).wait_recv()

            if halved(n):
                for dg in range(1, n_gr):
                    pair(n, 2, dg, f).start()

        for way in range(2):

            @pl.when(sends(2, way, 1))
            def _(way=way):
                line(n, 2, way, 1).start()

    def forward(n, m, s):
        for way in range(2):

            @pl.when(gets(m, way, s))
            def _(way=way):
                landed(n, m, way, s).wait_recv()
                if s < n_fs - 1:

                    @pl.when(sends(m, way, s + 1))
                    def _():
                        line(n, m, way, s + 1).start()

                if m < 2 or halved(n):
                    o = f - s if way == 0 else f + s
                    for dg in range(1, n_gr):
                        pair(n, m, dg, o).start()

    def pairs_in(n):
        for m in range(2):
            for dg in range(1, n_gr):
                for o in range(n_fs):
                    pair_landed(n, m, dg, o).wait_recv()

    def halves(n, act):
        for dg in range(1, n_gr):
            for o in range(n_fs):

                @pl.when(held(o))
                def _(dg=dg, o=o):
                    act(n, 2, dg, o)

    def drain(n):
        if halved(n):
            halves(n, lambda *at: pair(*at).wait_send())
        for m in range(2):
            for dg in range(1, n_gr):
                for o in range(n_fs):
                    pair(n, m, dg, o).wait_send()
        for m in range(3):
            for way in range(2):
                for s in range(1, n_fs):

                    @pl.when(sends(m, way, s))
                    def _(m=m, way=way, s=s):
                        line(n, m, way, s).wait_send()

        for dg in range(n_gr):
            if halved(n):
                if dg == 0:

                    @pl.when(jnp.logical_or(owner != t, lane != g))
                    def _():
                        part(n, 0).wait_send()

            elif dg == 0:

                @pl.when(owner != t)
                def _():
                    part(n, 0).wait_send()

            else:
                part(n, dg).wait_send()

    owned, depth = prompt_ref.shape[1], prompt_ref.shape[2]
    across = (((1,), (1,)), ((), ()))

    def unit(rows):
        return rows * lax.rsqrt(jnp.mean(rows * rows, axis=-1, keepdims=True) + 1e-06)

    def hide(n, source):
        @pl.loop(0, n_tp // 2)
        def _(i):
            rows = source[pl.ds(2 * i, 2)].reshape(2 * owned, depth)
            gate = lax.dot_general(
                rows, outs[n][0][...], across, preferred_element_type=jnp.float32
            )
            upper = lax.dot_general(
                rows, outs[n][1][...], across, preferred_element_type=jnp.float32
            )
            units = (jax.nn.silu(gate) * upper).astype(jnp.bfloat16)
            hidden[pl.ds(2 * i, 2)] = units.reshape(2, owned, units.shape[1])

    pairs = n_tp // 2
    seat, core = t // 2, lax.rem(t, 2)

    def at_seat(j):
        return 2 * lax.rem(seat + 1 + j, pairs)

    def mate(n, j):
        return remote(
            parts.at[n, j],
            mate_in.at[n, j],
            mate_send.at[n, j],
            mate_recv.at[n, j],
            (g, f, t + 1 - 2 * core),
        )

    def share(n, j):
        return remote(
            sums.at[n, j],
            parts_in.at[n, j],
            sum_send.at[n, j],
            sum_recv.at[n, j],
            (g, f, at_seat(j) + core),
        )

    def term(n, units):
        tall = outs[n][2].shape[1]
        total = jnp.zeros((owned, depth), jnp.float32)
        for k in range(per):
            total += jnp.dot(
                units[:, k * tall : (k + 1) * tall],
                outs[n][2][k],
                preferred_element_type=jnp.float32,
            )
        return total.astype(jnp.bfloat16)

    def spread(n):
        for j in range(pairs):
            parts[n, j] = term(n, hidden[at_seat(j) + 1 - core])
            if j > 0:
                mate(n, j - 1).start()
        for j in range(pairs):
            mine = term(n, hidden[at_seat(j) + core]).astype(jnp.float32)
            if j == 0:
                mate(n, pairs - 1).start()
            mate(n, j).wait_recv()
            both = mine + mate_in[n, j].astype(jnp.float32)
            if j < pairs - 1:
                sums[n, j] = both.astype(jnp.bfloat16)
                share(n, j).start()
            else:
                kept[...] = both

    def collect(n):
        total = kept[...]
        for j in range(pairs - 1):
            share(n, j).wait_recv()
            total += parts_in[n, j].astype(jnp.float32)
        return total

    def give(i):
        to = lax.rem(t + 1 + i, n_tp)
        return remote(
            normed_all.at[t], normed_all.at[t], row_send.at[i], row_recv.at[i], (g, f, to)
        )

    def given(i):
        src = lax.rem(t - 1 - i + n_tp, n_tp)
        return remote(
            normed_all.at[src], normed_all.at[src], row_send.at[i], row_recv.at[i], (g, f, src)
        )

    start_own(0)

    @pl.loop(0, n_tp)
    def _(i):
        normed[i] = unit(prompt_ref[i].astype(jnp.float32)).astype(jnp.bfloat16)

    start_down(0)
    for m in range(3):
        forward(0, m, 1)
    start_own(1)
    for s in range(2, n_fs):
        for m in range(3):
            forward(0, m, s)
    start_down(1)
    pairs_in(0)
    hide(0, normed)
    for m in range(3):
        forward(1, m, 1)
    spread(0)
    for s in range(2, n_fs - 1):
        for m in range(3):
            forward(1, m, s)
    stream[...] = prompt_ref[t].astype(jnp.float32) + 0.5 * collect(0)
    normed_all[t] = unit(stream[...]).astype(jnp.bfloat16)
    for m in range(2):
        forward(1, m, n_fs - 1)
    for i in range(n_tp - 1):
        give(i).start()
    for i in range(n_tp - 1):
        given(i).wait_recv()
    pairs_in(1)
    hide(1, normed_all)
    forward(1, 2, n_fs - 1)
    halves(1, lambda *at: pair_landed(*at).wait_recv())
    spread(1)
    drain(0)
    drain(1)
    mixed_ref[...] = (stream[...] + 0.5 * collect(1)).astype(jnp.bfloat16)
    for i in range(n_tp - 1):
        give(i).wait_send()
    for n in range(2):
        for j in range(pairs):
            mate(n, j).wait_send()
            if j < pairs - 1:
                share(n, j).wait_send()


def fused(sizes, prompt, *weights):
    n_gr, n_fs, n_tp = sizes
    per = n_gr * n_fs // n_tp
    tokens, depth = prompt.shape
    owned = tokens // n_tp
    rows, width = weights[1].shape
    tall, cols = weights[3].shape
    vmem = pl.BlockSpec(memory_space=pltpu.VMEM)
    dma = pltpu.SemaphoreType.DMA
    across = pltpu.VMEM((width, n_gr * n_fs * rows), jnp.bfloat16)
    down = pltpu.VMEM((per, tall, n_tp * cols), jnp.bfloat16)
    operands = [prompt.reshape(n_tp, owned, depth)]
    for n in range(2):
        gain, gate, up, tall_block = weights[4 * n : 4 * n + 4]
        operands += [gain[None, :], gate.T, up.T, tall_block]
    *served, mixed = pl.pallas_call(
        functools.partial(fused_kernel, n_gr, n_fs, n_tp),
        out_shape=(across, across, down) * 2
        + (jax.ShapeDtypeStruct((owned, depth), jnp.bfloat16),),
        in_specs=[vmem] * 9,
        out_specs=(vmem,) * 7,
        scratch_shapes=[
            pltpu.VMEM((2, tall, cols), jnp.bfloat16),
            pltpu.VMEM((n_tp, owned, depth), jnp.bfloat16),
            pltpu.VMEM((n_tp, owned, depth), jnp.bfloat16),
            pltpu.VMEM((n_tp, owned, width), jnp.bfloat16),
            pltpu.VMEM((2, n_tp // 2, owned, depth), jnp.bfloat16),
            pltpu.VMEM((2, n_tp // 2, owned, depth), jnp.bfloat16),
            pltpu.VMEM((2, n_tp // 2, owned, depth), jnp.bfloat16),
            pltpu.VMEM((2, n_tp // 2, owned, depth), jnp.bfloat16),
            pltpu.VMEM((owned, depth), jnp.float32),
            pltpu.VMEM((owned, depth), jnp.float32),
            dma((2, 3, 2, n_fs)),
            dma((2, 3, 2, n_fs)),
            dma((2, 3, n_gr, n_fs)),
            dma((2, 3, n_gr, n_fs)),
            dma((2, n_gr)),
            dma((2, n_tp)),
            dma((2, n_tp // 2)),
            dma((2, n_tp // 2)),
            dma((2, n_tp // 2)),
            dma((2, n_tp // 2)),
            dma((n_tp - 1,)),
            dma((n_tp - 1,)),
        ],
        compiler_params=pltpu.CompilerParams(
            collective_id=2, has_side_effects=True, vmem_limit_bytes=40 * 2**20
        ),
    )(*operands)
    gate_a, up_a, down_a, gate_b, up_b, down_b = served

    def flat(a):
        return a.reshape(per * tall, n_tp * cols)

    return (gate_a.T, up_a.T, flat(down_a), gate_b.T, up_b.T, flat(down_b), mixed)


def normalize(rows):
    rows = rows.astype(jnp.float32)
    scale = lax.rsqrt(jnp.mean(rows * rows, axis=-1, keepdims=True) + 1e-06)
    return (rows * scale).astype(jnp.bfloat16)


def hidden_units(normed, w_gate, w_up):
    gate = jnp.dot(normed, w_gate, preferred_element_type=jnp.float32)
    upper = jnp.dot(normed, w_up, preferred_element_type=jnp.float32)
    return (jax.nn.silu(gate) * upper).astype(jnp.bfloat16)


def rounded_term(hidden, w_down):
    return jnp.dot(hidden, w_down, preferred_element_type=jnp.float32).astype(jnp.bfloat16)


def shards(
    sizes,
    prompt,
    gain_first,
    gate_first,
    up_first,
    down_first,
    gain_second,
    gate_second,
    up_second,
    down_second,
):
    if gate_first.shape[0] % 128 == 0 and sizes[2] % 2 == 0:
        return fused(
            sizes,
            prompt,
            gain_first,
            gate_first,
            up_first,
            down_first,
            gain_second,
            gate_second,
            up_second,
            down_second,
        )
    gate_a, up_a, down_a = gather(sizes, 0, gain_first, gate_first, up_first, down_first)
    hidden_a = hidden_units(normalize(prompt), gate_a, up_a)
    term_a = rounded_term(hidden_a, down_a)
    term_a, gain_second = lax.optimization_barrier((term_a, gain_second))
    branch_a = lax.psum(term_a, "tp").astype(jnp.float32)
    gate_b, up_b, down_b = gather(sizes, 1, gain_second, gate_second, up_second, down_second)
    stream = prompt.astype(jnp.float32) + 0.5 * branch_a
    hidden_b = hidden_units(normalize(stream), gate_b, up_b)
    owned = hidden_b.shape[0] // lax.axis_size("tp")
    branch_b = lax.psum_scatter(
        rounded_term(hidden_b, down_b), "tp", scatter_dimension=0, tiled=True
    ).astype(jnp.float32)
    own_stream = lax.dynamic_slice_in_dim(stream, lax.axis_index("tp") * owned, owned, 0)
    mixed = (own_stream + 0.5 * branch_b).astype(jnp.bfloat16)
    return (gate_a, up_a, down_a, gate_b, up_b, down_b, mixed)


def solution(mesh):
    sizes = (mesh.shape["gr"], mesh.shape["fs"], mesh.shape["tp"])
    return jax.shard_map(
        functools.partial(shards, sizes),
        mesh=mesh,
        in_specs=(
            P(("gr", "fs"), None),
            P(("gr", "fs")),
            P(("gr", "fs"), "tp"),
            P(("gr", "fs"), "tp"),
            P(("gr", "fs"), "tp"),
            P(("gr", "fs")),
            P(("gr", "fs"), "tp"),
            P(("gr", "fs"), "tp"),
            P(("gr", "fs"), "tp"),
        ),
        out_specs=(
            P(None, "tp"),
            P(None, "tp"),
            P("tp", None),
            P(None, "tp"),
            P(None, "tp"),
            P("tp", None),
            P(("gr", "fs", "tp"), None),
        ),
        check_vma=False,
    )
```

```python
import functools

import jax
import jax.numpy as jnp
from jax import lax
from jax.experimental import pallas as pl
from jax.experimental.pallas import tpu as pltpu
from jax.sharding import PartitionSpec as P

MESH = pl.DeviceIdType.MESH


def gather_kernel(
    n_gr,
    n_fs,
    n_tp,
    gain_ref,
    gate_ref,
    up_ref,
    down_ref,
    gate_out,
    up_out,
    down_out,
    down_own,
    line_send,
    line_recv,
    pair_send,
    pair_recv,
    part_send,
    part_recv,
):
    g, f, t = lax.axis_index("gr"), lax.axis_index("fs"), lax.axis_index("tp")
    per = n_gr * n_fs // n_tp
    cols = down_ref.shape[1]
    first = lax.rem(t * per, n_fs)
    home = (t * per) // n_fs
    row = g * n_fs + f
    owner = row // per
    slot = lax.rem(row, per)

    width = gate_ref.shape[1]

    def place(ref, origin):
        if len(ref.shape) == 3:
            return ref.at[origin]
        return ref.at[:, pl.ds(pl.multiple_of(origin * width, 128), width)]

    gain = gain_ref[...]
    place(gate_out, row)[...] = (gain * gate_ref[...]).astype(jnp.bfloat16)
    place(up_out, row)[...] = (gain * up_ref[...]).astype(jnp.bfloat16)
    down_own[...] = down_ref[...].astype(jnp.bfloat16)

    @pl.when(owner == t)
    def _():
        down_out[slot, :, pl.ds(pl.multiple_of(t * cols, 128), cols)] = down_ref[...].astype(
            jnp.bfloat16
        )

    barrier = pltpu.get_barrier_semaphore()
    for dg in range(n_gr):
        for dt in range(n_tp):
            if dg or dt:
                pl.semaphore_signal(
                    barrier,
                    inc=1,
                    device_id=(lax.rem(g + dg, n_gr), f, lax.rem(t + dt, n_tp)),
                    device_id_type=MESH,
                )

    for near in (lax.rem(f + 1, n_fs), lax.rem(f + n_fs - 1, n_fs)):
        pl.semaphore_signal(barrier, inc=1, device_id=(g, near, t), device_id_type=MESH)
    pl.semaphore_wait(barrier, n_gr * n_tp + 1)

    outs = (gate_out, up_out)

    def held(o):
        return jnp.logical_and(o >= first, o < first + per)

    def block(m, o):
        if m < 2:
            return place(outs[m], g * n_fs + o)
        return down_out.at[o - first]

    def line(m, way, s):
        step = 1 if way == 0 else -1
        o = f - step * (s - 1)
        return pltpu.make_async_remote_copy(
            src_ref=block(m, o),
            dst_ref=block(m, o),
            send_sem=line_send.at[m, way, s],
            recv_sem=line_recv.at[m, way, s],
            device_id=(g, f + step, t),
            device_id_type=MESH,
        )

    def sends(m, way, s):
        step = 1 if way == 0 else -1
        o = f - step * (s - 1)
        fine = (f < n_fs - 1, o >= 0) if way == 0 else (f > 0, o <= n_fs - 1)
        ok = jnp.logical_and(*fine)
        return jnp.logical_and(ok, held(o)) if m == 2 else ok

    def gets(m, way, s):
        o = f - s if way == 0 else f + s
        ok = o >= 0 if way == 0 else o <= n_fs - 1
        return jnp.logical_and(ok, held(o)) if m == 2 else ok

    def landed(m, way, s):
        o = f - s if way == 0 else f + s
        return pltpu.make_async_remote_copy(
            src_ref=block(m, o),
            dst_ref=block(m, o),
            send_sem=line_send.at[m, way, s],
            recv_sem=line_recv.at[m, way, s],
            device_id=(g, f, t),
            device_id_type=MESH,
        )

    def pair(m, dg, o):
        return pltpu.make_async_remote_copy(
            src_ref=place(outs[m], g * n_fs + o),
            dst_ref=place(outs[m], g * n_fs + o),
            send_sem=pair_send.at[m, dg, o],
            recv_sem=pair_recv.at[m, dg, o],
            device_id=(lax.rem(g + dg, n_gr), f, t),
            device_id_type=MESH,
        )

    def pair_landed(m, dg, o):
        src = lax.rem(g - dg + n_gr, n_gr)
        return pltpu.make_async_remote_copy(
            src_ref=place(outs[m], src * n_fs + o),
            dst_ref=place(outs[m], src * n_fs + o),
            send_sem=pair_send.at[m, dg, o],
            recv_sem=pair_recv.at[m, dg, o],
            device_id=(src, f, t),
            device_id_type=MESH,
        )

    def part(dg):
        to = lax.rem(g + dg, n_gr)
        return pltpu.make_async_remote_copy(
            src_ref=down_own,
            dst_ref=down_out.at[slot, :, pl.ds(pl.multiple_of(t * cols, 128), cols)],
            send_sem=part_send.at[dg],
            recv_sem=part_recv.at[t],
            device_id=(to, f, owner),
            device_id_type=MESH,
        )

    def part_landed(src):
        return pltpu.make_async_remote_copy(
            src_ref=down_own,
            dst_ref=down_out.at[f - first, :, pl.ds(src * cols, cols)],
            send_sem=part_send.at[0],
            recv_sem=part_recv.at[src],
            device_id=(home, f, src),
            device_id_type=MESH,
        )

    for m in range(2):
        for way in range(2):

            @pl.when(sends(m, way, 1))
            def _(m=m, way=way):
                line(m, way, 1).start()

        for dg in range(1, n_gr):
            pair(m, dg, f).start()
    for dg in range(n_gr):
        if dg == 0:

            @pl.when(owner != t)
            def _():
                part(0).start()

        else:
            part(dg).start()

    @pl.when(held(f))
    def _():
        for src in range(n_tp):

            @pl.when(jnp.logical_or(home != g, t != src))
            def _(src=src):
                part_landed(src).wait_recv()

    for way in range(2):

        @pl.when(sends(2, way, 1))
        def _(way=way):
            line(2, way, 1).start()

    for s in range(1, n_fs):
        for m in range(3):
            for way in range(2):

                @pl.when(gets(m, way, s))
                def _(m=m, way=way, s=s):
                    landed(m, way, s).wait_recv()
                    if s < n_fs - 1:

                        @pl.when(sends(m, way, s + 1))
                        def _():
                            line(m, way, s + 1).start()

                    if m < 2:
                        o = f - s if way == 0 else f + s
                        for dg in range(1, n_gr):
                            pair(m, dg, o).start()

    for m in range(2):
        for dg in range(1, n_gr):
            for o in range(n_fs):
                pair_landed(m, dg, o).wait_recv()
                pair(m, dg, o).wait_send()
    for m in range(3):
        for way in range(2):
            for s in range(1, n_fs):

                @pl.when(sends(m, way, s))
                def _(m=m, way=way, s=s):
                    line(m, way, s).wait_send()

    for dg in range(n_gr):
        if dg == 0:

            @pl.when(owner != t)
            def _():
                part(0).wait_send()

        else:
            part(dg).wait_send()


def gather(sizes, call, gain, gate, up, down):
    n_gr, n_fs, n_tp = sizes
    per = n_gr * n_fs // n_tp
    rows, width = gate.shape
    wide = rows % 128 == 0
    whole = (width, n_gr * n_fs * rows) if wide else (n_gr * n_fs, width, rows)
    tall, cols = down.shape
    vmem = pl.BlockSpec(memory_space=pltpu.VMEM)
    dma = pltpu.SemaphoreType.DMA
    gate_all, up_all, down_all = pl.pallas_call(
        functools.partial(gather_kernel, n_gr, n_fs, n_tp),
        out_shape=(
            jax.ShapeDtypeStruct(whole, jnp.bfloat16),
            jax.ShapeDtypeStruct(whole, jnp.bfloat16),
            jax.ShapeDtypeStruct((per, tall, n_tp * cols), jnp.bfloat16),
        ),
        in_specs=[vmem] * 4,
        out_specs=(vmem,) * 3,
        scratch_shapes=[
            pltpu.VMEM((tall, cols), jnp.bfloat16),
            dma((3, 2, n_fs)),
            dma((3, 2, n_fs)),
            dma((2, n_gr, n_fs)),
            dma((2, n_gr, n_fs)),
            dma((n_gr,)),
            dma((n_tp,)),
        ],
        compiler_params=pltpu.CompilerParams(
            collective_id=call, has_side_effects=True, vmem_limit_bytes=32 * 2**20
        ),
        cost_estimate=pl.CostEstimate(
            flops=10**10, bytes_accessed=16 * 2**20, transcendentals=0
        ),
    )(gain[None, :], gate.T, up.T, down)

    def upright(a):
        return a.T if wide else a.transpose(0, 2, 1).reshape(n_gr * n_fs * rows, width)

    return (
        upright(gate_all),
        upright(up_all),
        down_all.reshape(per * tall, n_tp * cols),
    )


def fused_kernel(
    n_gr,
    n_fs,
    n_tp,
    prompt_ref,
    gain_a,
    gate_a,
    up_a,
    down_a,
    gain_b,
    gate_b,
    up_b,
    down_b,
    gate_out_a,
    up_out_a,
    down_out_a,
    gate_out_b,
    up_out_b,
    down_out_b,
    mixed_ref,
    down_own,
    normed,
    normed_all,
    hidden,
    parts,
    mate_in,
    sums,
    parts_in,
    kept,
    stream,
    line_send,
    line_recv,
    pair_send,
    pair_recv,
    part_send,
    part_recv,
    mate_send,
    mate_recv,
    sum_send,
    sum_recv,
    row_send,
    row_recv,
):
    g, f, t = lax.axis_index("gr"), lax.axis_index("fs"), lax.axis_index("tp")
    per = n_gr * n_fs // n_tp
    cols = down_a.shape[1]
    width = gate_a.shape[1]
    first = lax.rem(t * per, n_fs)
    home = (t * per) // n_fs
    row = g * n_fs + f
    owner = row // per
    slot = lax.rem(row, per)
    half = n_tp * cols // n_gr
    lane = t * n_gr // n_tp
    outs = ((gate_out_a, up_out_a, down_out_a), (gate_out_b, up_out_b, down_out_b))

    def halved(n):
        return n == 1

    def place(ref, origin):
        return ref.at[:, pl.ds(pl.multiple_of(origin * width, 128), width)]

    for n, (gain, gate, up, down) in enumerate(
        ((gain_a, gate_a, up_a, down_a), (gain_b, gate_b, up_b, down_b))
    ):
        place(outs[n][0], row)[...] = (gain[...] * gate[...]).astype(jnp.bfloat16)
        place(outs[n][1], row)[...] = (gain[...] * up[...]).astype(jnp.bfloat16)
        down_own[n] = down[...].astype(jnp.bfloat16)

        @pl.when(jnp.logical_and(owner == t, lane == g) if halved(n) else owner == t)
        def _(n=n, down=down):
            outs[n][2][slot, :, pl.ds(pl.multiple_of(t * cols, 128), cols)] = down[...].astype(
                jnp.bfloat16
            )

    barrier = pltpu.get_barrier_semaphore()
    for dg in range(n_gr):
        for dt in range(n_tp):
            if dg or dt:
                pl.semaphore_signal(
                    barrier,
                    inc=1,
                    device_id=(lax.rem(g + dg, n_gr), f, lax.rem(t + dt, n_tp)),
                    device_id_type=MESH,
                )
    for near in (lax.rem(f + 1, n_fs), lax.rem(f + n_fs - 1, n_fs)):
        pl.semaphore_signal(barrier, inc=1, device_id=(g, near, t), device_id_type=MESH)
    pl.semaphore_wait(barrier, n_gr * n_tp + 1)

    def held(o):
        return jnp.logical_and(o >= first, o < first + per)

    def remote(src, dst, send, recv, to):
        return pltpu.make_async_remote_copy(
            src_ref=src,
            dst_ref=dst,
            send_sem=send,
            recv_sem=recv,
            device_id=to,
            device_id_type=MESH,
        )

    def block(n, m, o):
        if m < 2:
            return place(outs[n][m], g * n_fs + o)
        if halved(n):
            return share_of(n, o, g)
        return outs[n][2].at[o - first]

    def share_of(n, o, column):
        return outs[n][2].at[o - first, :, pl.ds(pl.multiple_of(column * half, 128), half)]

    def line(n, m, way, s):
        step = 1 if way == 0 else -1
        o = f - step * (s - 1)
        sems = line_send.at[n, m, way, s], line_recv.at[n, m, way, s]
        return remote(block(n, m, o), block(n, m, o), *sems, (g, f + step, t))

    def sends(m, way, s):
        step = 1 if way == 0 else -1
        o = f - step * (s - 1)
        fine = (f < n_fs - 1, o >= 0) if way == 0 else (f > 0, o <= n_fs - 1)
        ok = jnp.logical_and(*fine)
        return jnp.logical_and(ok, held(o)) if m == 2 else ok

    def gets(m, way, s):
        o = f - s if way == 0 else f + s
        ok = o >= 0 if way == 0 else o <= n_fs - 1
        return jnp.logical_and(ok, held(o)) if m == 2 else ok

    def landed(n, m, way, s):
        o = f - s if way == 0 else f + s
        sems = line_send.at[n, m, way, s], line_recv.at[n, m, way, s]
        return remote(block(n, m, o), block(n, m, o), *sems, (g, f, t))

    def pair(n, m, dg, o):
        spot = share_of(n, o, g) if m == 2 else place(outs[n][m], g * n_fs + o)
        sems = pair_send.at[n, m, dg, o], pair_recv.at[n, m, dg, o]
        return remote(spot, spot, *sems, (lax.rem(g + dg, n_gr), f, t))

    def pair_landed(n, m, dg, o):
        src = lax.rem(g - dg + n_gr, n_gr)
        spot = share_of(n, o, src) if m == 2 else place(outs[n][m], src * n_fs + o)
        sems = pair_send.at[n, m, dg, o], pair_recv.at[n, m, dg, o]
        return remote(spot, spot, *sems, (src, f, t))

    def part(n, dg):
        return remote(
            down_own.at[n],
            outs[n][2].at[slot, :, pl.ds(pl.multiple_of(t * cols, 128), cols)],
            part_send.at[n, dg],
            part_recv.at[n, t],
            (lane if halved(n) else lax.rem(g + dg, n_gr), f, owner),
        )

    def part_landed(n, src):
        return remote(
            down_own.at[n],
            outs[n][2].at[f - first, :, pl.ds(src * cols, cols)],
            part_send.at[n, 0],
            part_recv.at[n, src],
            (home, f, src),
        )

    def start_own(n):
        for m in range(2):
            for way in range(2):

                @pl.when(sends(m, way, 1))
                def _(m=m, way=way):
                    line(n, m, way, 1).start()

            for dg in range(1, n_gr):
                pair(n, m, dg, f).start()
        for dg in range(n_gr):
            if halved(n):
                if dg == 0:

                    @pl.when(jnp.logical_or(owner != t, lane != g))
                    def _():
                        part(n, 0).start()

            elif dg == 0:

                @pl.when(owner != t)
                def _():
                    part(n, 0).start()

            else:
                part(n, dg).start()

    def start_down(n):
        @pl.when(held(f))
        def _():
            for src in range(n_tp):

                away = jnp.logical_or(home != g, t != src)
                if halved(n):
                    away = jnp.logical_and(away, g == src * n_gr // n_tp)

                @pl.when(away)
                def _(src=src):
                    part_landed(n, src).wait_recv()

            if halved(n):
                for dg in range(1, n_gr):
                    pair(n, 2, dg, f).start()

        for way in range(2):

            @pl.when(sends(2, way, 1))
            def _(way=way):
                line(n, 2, way, 1).start()

    def forward(n, m, s):
        for way in range(2):

            @pl.when(gets(m, way, s))
            def _(way=way):
                landed(n, m, way, s).wait_recv()
                if s < n_fs - 1:

                    @pl.when(sends(m, way, s + 1))
                    def _():
                        line(n, m, way, s + 1).start()

                if m < 2 or halved(n):
                    o = f - s if way == 0 else f + s
                    for dg in range(1, n_gr):
                        pair(n, m, dg, o).start()

    def pairs_in(n):
        for m in range(2):
            for dg in range(1, n_gr):
                for o in range(n_fs):
                    pair_landed(n, m, dg, o).wait_recv()

    def halves(n, act):
        for dg in range(1, n_gr):
            for o in range(n_fs):

                @pl.when(held(o))
                def _(dg=dg, o=o):
                    act(n, 2, dg, o)

    def drain(n):
        if halved(n):
            halves(n, lambda *at: pair(*at).wait_send())
        for m in range(2):
            for dg in range(1, n_gr):
                for o in range(n_fs):
                    pair(n, m, dg, o).wait_send()
        for m in range(3):
            for way in range(2):
                for s in range(1, n_fs):

                    @pl.when(sends(m, way, s))
                    def _(m=m, way=way, s=s):
                        line(n, m, way, s).wait_send()

        for dg in range(n_gr):
            if halved(n):
                if dg == 0:

                    @pl.when(jnp.logical_or(owner != t, lane != g))
                    def _():
                        part(n, 0).wait_send()

            elif dg == 0:

                @pl.when(owner != t)
                def _():
                    part(n, 0).wait_send()

            else:
                part(n, dg).wait_send()

    owned, depth = prompt_ref.shape[1], prompt_ref.shape[2]
    across = (((1,), (1,)), ((), ()))

    def unit(rows):
        return rows * lax.rsqrt(jnp.mean(rows * rows, axis=-1, keepdims=True) + 1e-06)

    def hide(n, source):
        @pl.loop(0, n_tp // 2)
        def _(i):
            rows = source[pl.ds(2 * i, 2)].reshape(2 * owned, depth)
            gate = lax.dot_general(
                rows, outs[n][0][...], across, preferred_element_type=jnp.float32
            )
            upper = lax.dot_general(
                rows, outs[n][1][...], across, preferred_element_type=jnp.float32
            )
            units = (jax.nn.silu(gate) * upper).astype(jnp.bfloat16)
            hidden[pl.ds(2 * i, 2)] = units.reshape(2, owned, units.shape[1])

    pairs = n_tp // 2
    seat, core = t // 2, lax.rem(t, 2)

    def at_seat(j):
        return 2 * lax.rem(seat + 1 + j, pairs)

    def mate(n, j):
        return remote(
            parts.at[n, j],
            mate_in.at[n, j],
            mate_send.at[n, j],
            mate_recv.at[n, j],
            (g, f, t + 1 - 2 * core),
        )

    def share(n, j):
        return remote(
            sums.at[n, j],
            parts_in.at[n, j],
            sum_send.at[n, j],
            sum_recv.at[n, j],
            (g, f, at_seat(j) + core),
        )

    def term(n, units):
        tall = outs[n][2].shape[1]
        total = jnp.zeros((owned, depth), jnp.float32)
        for k in range(per):
            total += jnp.dot(
                units[:, k * tall : (k + 1) * tall],
                outs[n][2][k],
                preferred_element_type=jnp.float32,
            )
        return total.astype(jnp.bfloat16)

    def spread(n):
        for j in range(pairs):
            parts[n, j] = term(n, hidden[at_seat(j) + 1 - core])
            if j > 0:
                mate(n, j - 1).start()
        for j in range(pairs):
            mine = term(n, hidden[at_seat(j) + core]).astype(jnp.float32)
            if j == 0:
                mate(n, pairs - 1).start()
            mate(n, j).wait_recv()
            both = mine + mate_in[n, j].astype(jnp.float32)
            if j < pairs - 1:
                sums[n, j] = both.astype(jnp.bfloat16)
                share(n, j).start()
            else:
                kept[...] = both

    def collect(n):
        total = kept[...]
        for j in range(pairs - 1):
            share(n, j).wait_recv()
            total += parts_in[n, j].astype(jnp.float32)
        return total

    def give(i):
        to = lax.rem(t + 1 + i, n_tp)
        return remote(
            normed_all.at[t], normed_all.at[t], row_send.at[i], row_recv.at[i], (g, f, to)
        )

    def given(i):
        src = lax.rem(t - 1 - i + n_tp, n_tp)
        return remote(
            normed_all.at[src], normed_all.at[src], row_send.at[i], row_recv.at[i], (g, f, src)
        )

    start_own(0)

    @pl.loop(0, n_tp)
    def _(i):
        normed[i] = unit(prompt_ref[i].astype(jnp.float32)).astype(jnp.bfloat16)

    start_down(0)
    for m in range(3):
        forward(0, m, 1)
    start_own(1)
    for s in range(2, n_fs):
        for m in range(3):
            forward(0, m, s)
    start_down(1)
    for m in range(3):
        forward(1, m, 1)
    pairs_in(0)
    hide(0, normed)
    spread(0)
    for s in range(2, n_fs - 1):
        for m in range(3):
            forward(1, m, s)
    stream[...] = prompt_ref[t].astype(jnp.float32) + 0.5 * collect(0)
    normed_all[t] = unit(stream[...]).astype(jnp.bfloat16)
    for m in range(2):
        forward(1, m, n_fs - 1)
    for i in range(n_tp - 1):
        give(i).start()
    for i in range(n_tp - 1):
        given(i).wait_recv()
    pairs_in(1)
    forward(1, 2, n_fs - 1)
    hide(1, normed_all)
    halves(1, lambda *at: pair_landed(*at).wait_recv())
    spread(1)
    drain(0)
    drain(1)
    mixed_ref[...] = (stream[...] + 0.5 * collect(1)).astype(jnp.bfloat16)
    for i in range(n_tp - 1):
        give(i).wait_send()
    for n in range(2):
        for j in range(pairs):
            mate(n, j).wait_send()
            if j < pairs - 1:
                share(n, j).wait_send()


def fused(sizes, prompt, *weights):
    n_gr, n_fs, n_tp = sizes
    per = n_gr * n_fs // n_tp
    tokens, depth = prompt.shape
    owned = tokens // n_tp
    rows, width = weights[1].shape
    tall, cols = weights[3].shape
    vmem = pl.BlockSpec(memory_space=pltpu.VMEM)
    dma = pltpu.SemaphoreType.DMA
    across = pltpu.VMEM((width, n_gr * n_fs * rows), jnp.bfloat16)
    down = pltpu.VMEM((per, tall, n_tp * cols), jnp.bfloat16)
    operands = [prompt.reshape(n_tp, owned, depth)]
    for n in range(2):
        gain, gate, up, tall_block = weights[4 * n : 4 * n + 4]
        operands += [gain[None, :], gate.T, up.T, tall_block]
    *served, mixed = pl.pallas_call(
        functools.partial(fused_kernel, n_gr, n_fs, n_tp),
        out_shape=(across, across, down) * 2
        + (jax.ShapeDtypeStruct((owned, depth), jnp.bfloat16),),
        in_specs=[vmem] * 9,
        out_specs=(vmem,) * 7,
        scratch_shapes=[
            pltpu.VMEM((2, tall, cols), jnp.bfloat16),
            pltpu.VMEM((n_tp, owned, depth), jnp.bfloat16),
            pltpu.VMEM((n_tp, owned, depth), jnp.bfloat16),
            pltpu.VMEM((n_tp, owned, width), jnp.bfloat16),
            pltpu.VMEM((2, n_tp // 2, owned, depth), jnp.bfloat16),
            pltpu.VMEM((2, n_tp // 2, owned, depth), jnp.bfloat16),
            pltpu.VMEM((2, n_tp // 2, owned, depth), jnp.bfloat16),
            pltpu.VMEM((2, n_tp // 2, owned, depth), jnp.bfloat16),
            pltpu.VMEM((owned, depth), jnp.float32),
            pltpu.VMEM((owned, depth), jnp.float32),
            dma((2, 3, 2, n_fs)),
            dma((2, 3, 2, n_fs)),
            dma((2, 3, n_gr, n_fs)),
            dma((2, 3, n_gr, n_fs)),
            dma((2, n_gr)),
            dma((2, n_tp)),
            dma((2, n_tp // 2)),
            dma((2, n_tp // 2)),
            dma((2, n_tp // 2)),
            dma((2, n_tp // 2)),
            dma((n_tp - 1,)),
            dma((n_tp - 1,)),
        ],
        compiler_params=pltpu.CompilerParams(
            collective_id=2, has_side_effects=True, vmem_limit_bytes=40 * 2**20
        ),
    )(*operands)
    gate_a, up_a, down_a, gate_b, up_b, down_b = served

    def flat(a):
        return a.reshape(per * tall, n_tp * cols)

    return (gate_a.T, up_a.T, flat(down_a), gate_b.T, up_b.T, flat(down_b), mixed)


def normalize(rows):
    rows = rows.astype(jnp.float32)
    scale = lax.rsqrt(jnp.mean(rows * rows, axis=-1, keepdims=True) + 1e-06)
    return (rows * scale).astype(jnp.bfloat16)


def hidden_units(normed, w_gate, w_up):
    gate = jnp.dot(normed, w_gate, preferred_element_type=jnp.float32)
    upper = jnp.dot(normed, w_up, preferred_element_type=jnp.float32)
    return (jax.nn.silu(gate) * upper).astype(jnp.bfloat16)


def rounded_term(hidden, w_down):
    return jnp.dot(hidden, w_down, preferred_element_type=jnp.float32).astype(jnp.bfloat16)


def shards(
    sizes,
    prompt,
    gain_first,
    gate_first,
    up_first,
    down_first,
    gain_second,
    gate_second,
    up_second,
    down_second,
):
    if gate_first.shape[0] % 128 == 0 and sizes[2] % 2 == 0:
        return fused(
            sizes,
            prompt,
            gain_first,
            gate_first,
            up_first,
            down_first,
            gain_second,
            gate_second,
            up_second,
            down_second,
        )
    gate_a, up_a, down_a = gather(sizes, 0, gain_first, gate_first, up_first, down_first)
    hidden_a = hidden_units(normalize(prompt), gate_a, up_a)
    term_a = rounded_term(hidden_a, down_a)
    term_a, gain_second = lax.optimization_barrier((term_a, gain_second))
    branch_a = lax.psum(term_a, "tp").astype(jnp.float32)
    gate_b, up_b, down_b = gather(sizes, 1, gain_second, gate_second, up_second, down_second)
    stream = prompt.astype(jnp.float32) + 0.5 * branch_a
    hidden_b = hidden_units(normalize(stream), gate_b, up_b)
    owned = hidden_b.shape[0] // lax.axis_size("tp")
    branch_b = lax.psum_scatter(
        rounded_term(hidden_b, down_b), "tp", scatter_dimension=0, tiled=True
    ).astype(jnp.float32)
    own_stream = lax.dynamic_slice_in_dim(stream, lax.axis_index("tp") * owned, owned, 0)
    mixed = (own_stream + 0.5 * branch_b).astype(jnp.bfloat16)
    return (gate_a, up_a, down_a, gate_b, up_b, down_b, mixed)


def solution(mesh):
    sizes = (mesh.shape["gr"], mesh.shape["fs"], mesh.shape["tp"])
    return jax.shard_map(
        functools.partial(shards, sizes),
        mesh=mesh,
        in_specs=(
            P(("gr", "fs"), None),
            P(("gr", "fs")),
            P(("gr", "fs"), "tp"),
            P(("gr", "fs"), "tp"),
            P(("gr", "fs"), "tp"),
            P(("gr", "fs")),
            P(("gr", "fs"), "tp"),
            P(("gr", "fs"), "tp"),
            P(("gr", "fs"), "tp"),
        ),
        out_specs=(
            P(None, "tp"),
            P(None, "tp"),
            P("tp", None),
            P(None, "tp"),
            P(None, "tp"),
            P("tp", None),
            P(("gr", "fs", "tp"), None),
        ),
        check_vma=False,
    )
```
